32 devices in a mesh: sp: 8 (over z, x), tp: 4 (over y, core).
Axes of the slice: x: 2, y: 2, z: 4, core: 2. Of those that a mesh axis runs over, the one named last changes fastest.
Arguments:
- resid: bfloat16 [2048, 4096], P(('sp', 'tp')), may hold values from -6 to 6
- queries: bfloat16 [2048, 2048], P('sp', 'tp'), may hold values from -6 to 6
- keys: bfloat16 [2048, 512], P('sp', 'tp'), may hold values from -6 to 6
- values: bfloat16 [2048, 512], P('sp', 'tp'), may hold values from -6 to 6
- q_gain: float32 [128], replicated, may hold values from 0.5 to 6
- key_norm_gain: float32 [128], replicated, may hold values from 0.5 to 6
- out_weight: bfloat16 [2048, 4096], P('tp'), may hold values from -0.125 to 0.125
- norm1_gain: float32 [4096], replicated, may hold values from 0.1 to 1.9
- norm2_gain: float32 [4096], replicated, may hold values from 0.1 to 1.9
- expert_ids: int32 [2048, 2], P(('sp', 'tp')), may hold values from 0 to 7, all different within a row; in each aligned block of 64 rows (0 to 63, 64 to 127, ...) at most 24 rows name the same one
- group_weight: float32 [2048], P(('sp', 'tp')), may hold values from 0.3 to 1
- expert_weight: float32 [2048, 2], P(('sp', 'tp')), may hold values from 0.1 to 1
- gate_proj: bfloat16 [8, 4096, 1024], P('sp', None, 'tp'), may hold values from -0.09375 to 0.09375
- up_proj: bfloat16 [8, 4096, 1024], P('sp', None, 'tp'), may hold values from -0.09375 to 0.09375
- down_proj: bfloat16 [8, 1024, 4096], P('sp', 'tp'), may hold values from -0.1875 to 0.1875
Outputs:
- mixed_out: bfloat16 [2048, 4096], P(('sp', 'tp'))
The draws below stay inside these ranges and needn't reach their ends.
Inputs may be any that keep to these rules, and one draw needn't show every extreme that they name: `expert_ids`: each row names 2 different experts. Among the rows of one device (aligned blocks of 64 rows) no expert is named by more than 24 rows, a bound that some block reaches.
All inputs are finite; a program needn't handle non-finite values.
Results may differ from the reference program's by a relative error of at most 0.012.
The reference program's roundings to bfloat16 on the way count: a program that leaves them out, or rounds other values in their place, can miss the bound.
Values may be sent and summed in bfloat16 or wider, within the bound.
A program may use at most 192 MiB of HBM per device.

```python
import math
import jax
import jax.numpy as jnp
import numpy as np
from jax import lax

D = 4096
HEAD_WIDTH = 128
QUERY_HEADS = 16
KEY_VALUE_HEADS = 4
GRID_W = 64
FF = 1024
TOP = 2
SEQUENCE_TOKENS = 2048
ROWS_DEV = 64
EXPERTS = 8
CAP = 24
N_SP = 8
N_TP = 4


def gain_law(key):
    return jax.random.uniform(key, (HEAD_WIDTH,), jnp.float32, 0.5, 2.0)


def draw_q_gain(key, part):
    return gain_law(jax.random.fold_in(key, 31))


def draw_key_norm_gain(key, part):
    return gain_law(jax.random.fold_in(key, 37))


def key_table(key):
    sampled_values = jax.random.normal(jax.random.fold_in(key, 41), (SEQUENCE_TOKENS, KEY_VALUE_HEADS * HEAD_WIDTH), jnp.float32)
    return jnp.clip(sampled_values, -6.0, 6.0)


def draw_keys(key, part):
    return key_table(key).astype(jnp.bfloat16)


def draw_queries(key, part):
    sampled_values = jax.random.normal(jax.random.fold_in(key, 43), (SEQUENCE_TOKENS, QUERY_HEADS * HEAD_WIDTH), jnp.float32)
    sampled_values = jnp.clip(sampled_values, -6.0, 6.0)
    return sampled_values.astype(jnp.bfloat16)


def block_scale(stream_key, shape, split, low, high):
    def one(dim, parts):
        draws = jax.random.uniform(jax.random.fold_in(jax.random.fold_in(stream_key, 6), dim), (parts,), jnp.float32, low / len(split), high / len(split))
        return jnp.repeat(jnp.exp(draws), shape[dim] // parts).reshape((-1,) + (1,) * (len(shape) - dim - 1))

    loudness = one(*split[0])
    for cut in split[1:]:
        loudness = loudness * one(*cut)
    return loudness


def routed_block(own_key, own, number, rows, amount, top, reach, lean):
    ranking = jax.random.permutation(own_key, amount)
    heavy_load, common = load_shares(amount, rows * top, reach, lean, True), load_shares(amount, rows * top, reach, lean, False)
    places = jnp.arange(amount)

    def named(tallies, turn):
        used = int((tallies > 0).sum())
        fixed = max(1, used // 4)
        shifted = fixed + (places - fixed + turn * (used - fixed)) % max(1, amount - fixed)
        return jnp.zeros((amount,), jnp.int32).at[ranking[jnp.where(places < fixed, places, shifted)]].set(jnp.asarray(tallies, jnp.int32))

    tallies = jnp.where(number % 4 == 0, named(heavy_load, number // 4), named(common, number - number // 4 - 1))
    mixed = jax.random.permutation(jax.random.fold_in(own, 3), amount)
    donor, sink = mixed[0:amount // 2 * 2:2], mixed[1:amount // 2 * 2:2]
    slack = jnp.minimum(tallies[donor] - 1, reach - tallies[sink]) // 2
    slack = jnp.where((donor == ranking[0]) | (sink == ranking[0]) | (tallies[sink] == 0), 0, jnp.maximum(slack, 0))
    shifted = jax.random.randint(jax.random.fold_in(own, 4), (amount // 2,), 0, 1 << 20) % (slack + 1)
    tallies = tallies.at[donor].add(-shifted).at[sink].add(shifted)
    items = jnp.searchsorted(jnp.cumsum(tallies), jnp.arange(rows * top), side="right").astype(jnp.int32)
    table = items.reshape(top, rows).T
    table = table[jax.random.permutation(jax.random.fold_in(own, 1), rows)]
    turn = jax.random.randint(jax.random.fold_in(own, 2), (rows, 1), 0, top)
    return jnp.take_along_axis(table, (jnp.arange(top)[None, :] + turn) % top, axis=1)


def load_shares(count, total, bound, skew, full):
    weights = [(1 << 20) // math.isqrt(grade ** skew) + 1 for grade in range(1, count + 1)]
    largest = bound if full else min(bound, max(-(-total // count), total * weights[0] // sum(weights)))
    least = 1 if total - largest >= count - 1 else 0
    holding, surplus = [largest] + [least] * (count - 1), total - largest - least * (count - 1)
    while surplus > 0:
        free = [i for i in range(1, count) if holding[i] < largest] or [i for i in range(1, count) if holding[i] < bound]
        whole, left = sum([weights[i] for i in free]), surplus
        for i in free:
            more = min(bound - holding[i], max(1, left * weights[i] // whole), surplus)
            holding[i] = holding[i] + more
            surplus = surplus - more
    return np.array(holding)


def normal_values(rng, dims, deviation, bound, split=(), kind=jnp.bfloat16):
    values = deviation * jax.random.normal(rng, dims, jnp.float32)
    if split:
        values = values * block_scale(rng, dims, split, -0.22, 0.18)
    return jnp.clip(values, -bound, bound).astype(kind)


def setup_inputs(seed: int = 0) -> dict:
    streams_of = jax.random.split(jax.random.key(seed), 16)
    resid = normal_values(streams_of[0], (SEQUENCE_TOKENS, D), 1.0, 6.0, ((0, 32),))
    queries = draw_queries(jax.random.fold_in(streams_of[15], 71), 0)
    keys = draw_keys(jax.random.fold_in(streams_of[15], 71), 0)
    values = normal_values(streams_of[3], (SEQUENCE_TOKENS, KEY_VALUE_HEADS * HEAD_WIDTH), 1.0, 6.0, ((0, 8), (1, 4)))
    q_gain = draw_q_gain(jax.random.fold_in(streams_of[15], 71), 0)
    key_norm_gain = draw_key_norm_gain(jax.random.fold_in(streams_of[15], 71), 0)
    out_weight = normal_values(streams_of[6], (QUERY_HEADS * HEAD_WIDTH, D), (QUERY_HEADS * HEAD_WIDTH) ** -0.5, 0.125, ((0, 4),))
    norm1_gain = jnp.clip(1.0 + 0.18 * jax.random.normal(streams_of[7], (D,), jnp.float32), 0.1, 1.9)
    norm2_gain = jnp.clip(1.0 + 0.18 * jax.random.normal(streams_of[8], (D,), jnp.float32), 0.1, 1.9)
    expert_ids_keys = jax.random.split(jax.random.fold_in(streams_of[9], 1), SEQUENCE_TOKENS // ROWS_DEV)
    expert_ids_turns = jax.random.permutation(jax.random.fold_in(streams_of[9], 3), SEQUENCE_TOKENS // ROWS_DEV)
    expert_ids = jax.vmap(lambda own, number: routed_block(jax.random.fold_in(streams_of[9], 2), own, number, ROWS_DEV, EXPERTS, TOP, CAP, 1))(expert_ids_keys, expert_ids_turns).reshape((SEQUENCE_TOKENS, TOP))
    group_weight = jnp.clip(0.3 + 0.7 * jax.random.uniform(streams_of[10], (SEQUENCE_TOKENS,), jnp.float32) ** block_scale(streams_of[10], (SEQUENCE_TOKENS,), ((0, 32),), -0.2, 0.2), 0.3, 1.0)
    expert_weight = jnp.clip(0.1 + 0.9 * jax.random.uniform(streams_of[11], (SEQUENCE_TOKENS, TOP), jnp.float32) ** block_scale(streams_of[11], (SEQUENCE_TOKENS, TOP), ((0, 32),), -0.2, 0.2), 0.1, 1.0)
    gate_proj = normal_values(streams_of[12], (EXPERTS, D, FF), D ** -0.5, 0.09375, ((0, 8), (2, 4)))
    up_proj = normal_values(streams_of[13], (EXPERTS, D, FF), D ** -0.5, 0.09375, ((0, 8), (2, 4)))
    down_proj = normal_values(streams_of[14], (EXPERTS, FF, D), FF ** -0.5, 0.1875, ((0, 8), (1, 4)))
    return dict(resid=resid, queries=queries, keys=keys, values=values, q_gain=q_gain, key_norm_gain=key_norm_gain, out_weight=out_weight, norm1_gain=norm1_gain, norm2_gain=norm2_gain, expert_ids=expert_ids, group_weight=group_weight, expert_weight=expert_weight, gate_proj=gate_proj, up_proj=up_proj, down_proj=down_proj)


deep_alpha = 2.0 ** 0.5
rope_theta = 10000.0

def apply_rotary_heads(block, gain, grid_positions):
    values32 = block.astype(jnp.float32)
    normed = values32 * lax.rsqrt(lax.optimization_barrier(jnp.mean(values32 * values32, -1, keepdims=True)) + 1e-06) * gain
    half = normed.shape[-1] // 2
    inv_freq = rope_theta ** (-jnp.arange(0, half, 2, dtype=jnp.float32) / half)
    grid_row = (grid_positions // GRID_W).astype(jnp.float32)
    grid_col = (grid_positions % GRID_W).astype(jnp.float32)
    angle = jnp.concatenate([grid_row[:, None] * inv_freq, grid_col[:, None] * inv_freq], -1)[:, None, :]
    cosine = jnp.cos(angle)
    sine = jnp.sin(angle)
    first = normed[..., :half]
    second = normed[..., half:]
    turned = jnp.concatenate([first * cosine - second * sine, first * sine + second * cosine], -1)
    return turned.astype(jnp.bfloat16)

def layer_norm_gain(summed, gain):
    centre = summed - lax.optimization_barrier(jnp.mean(summed, -1, keepdims=True))
    spread = lax.optimization_barrier(jnp.mean(centre * centre, -1, keepdims=True))
    return centre * lax.rsqrt(spread + 1e-06) * gain

def reference(resid, queries, keys, values, q_gain, key_norm_gain, out_weight, norm1_gain, norm2_gain, expert_ids, group_weight, expert_weight, gate_proj, up_proj, down_proj):
    grid_positions = jnp.arange(SEQUENCE_TOKENS, dtype=jnp.int32)
    query_group = QUERY_HEADS // KEY_VALUE_HEADS
    q_rot = apply_rotary_heads(queries.reshape(SEQUENCE_TOKENS, QUERY_HEADS, HEAD_WIDTH), q_gain, grid_positions)
    rotated_keys = apply_rotary_heads(keys.reshape(SEQUENCE_TOKENS, KEY_VALUE_HEADS, HEAD_WIDTH), key_norm_gain, grid_positions).astype(jnp.float32)
    value_rows_full = values.reshape(SEQUENCE_TOKENS, KEY_VALUE_HEADS, HEAD_WIDTH).astype(jnp.float32)
    query_extent = math.gcd(SEQUENCE_TOKENS, 128)

    def attend(query_tile):
        query_widened = query_tile.reshape(query_extent, KEY_VALUE_HEADS, query_group, HEAD_WIDTH).astype(jnp.float32)
        scores = jnp.einsum('qkgd,lkd->kgql', query_widened, rotated_keys) * HEAD_WIDTH ** (-0.5)
        row_max = lax.optimization_barrier(jnp.max(scores, -1, keepdims=True))
        weights = jnp.exp(scores - row_max)
        row_sum = lax.optimization_barrier(jnp.sum(weights, -1))
        rounded = lax.optimization_barrier(weights.astype(jnp.bfloat16)).astype(jnp.float32)
        mixed = jnp.einsum('kgql,lkd->qkgd', rounded, value_rows_full)
        mixed = mixed / jnp.transpose(row_sum, (2, 0, 1))[..., None]
        return mixed.reshape(query_extent, QUERY_HEADS * HEAD_WIDTH).astype(jnp.bfloat16)
    attn = lax.map(attend, q_rot.reshape(SEQUENCE_TOKENS // query_extent, query_extent, QUERY_HEADS, HEAD_WIDTH)).reshape(SEQUENCE_TOKENS, QUERY_HEADS * HEAD_WIDTH)
    proj = jnp.dot(attn, out_weight, preferred_element_type=jnp.float32).astype(jnp.bfloat16)
    summed = deep_alpha * resid.astype(jnp.float32) + proj.astype(jnp.float32)
    x_one = layer_norm_gain(summed, norm1_gain).astype(jnp.bfloat16)
    gates = group_weight[:, None] * expert_weight / lax.optimization_barrier(jnp.sum(expert_weight, -1, keepdims=True))
    copies = SEQUENCE_TOKENS * TOP
    most_rows = CAP * N_SP * N_TP
    ff_dev = FF // N_TP
    flat_ids = expert_ids.reshape(-1)
    gate_flat = jnp.concatenate([gates.reshape(-1), jnp.zeros((1,), jnp.float32)])
    x_padded = jnp.concatenate([x_one, jnp.zeros((1, D), jnp.bfloat16)], 0)

    def per_expert(total, expert):
        index = jnp.nonzero(flat_ids == expert, size=most_rows, fill_value=copies)[0].astype(jnp.int32)
        token_index = jnp.where(index < copies, index // TOP, SEQUENCE_TOKENS).astype(jnp.int32)
        chosen = x_padded[token_index]
        w_gate = lax.dynamic_index_in_dim(gate_proj, expert, 0, keepdims=False)
        w_up = lax.dynamic_index_in_dim(up_proj, expert, 0, keepdims=False)
        w_down = lax.dynamic_index_in_dim(down_proj, expert, 0, keepdims=False)
        gate_part = jnp.dot(chosen, w_gate, preferred_element_type=jnp.float32)
        up_part = jnp.dot(chosen, w_up, preferred_element_type=jnp.float32)
        hidden = (jax.nn.silu(gate_part) * up_part).astype(jnp.bfloat16)
        expert_sum = jnp.zeros((most_rows, D), jnp.float32)
        for lane in range(N_TP):
            partial_sum = jnp.dot(hidden[:, lane * ff_dev:(lane + 1) * ff_dev], w_down[lane * ff_dev:(lane + 1) * ff_dev], preferred_element_type=jnp.float32)
            rounded = lax.optimization_barrier(partial_sum.astype(jnp.bfloat16))
            expert_sum = expert_sum + rounded.astype(jnp.float32)
        expert_out = expert_sum.astype(jnp.bfloat16).astype(jnp.float32)
        weighted = gate_flat[index][:, None] * expert_out
        return (total.at[token_index].add(weighted), None)
    start_total = jnp.zeros((SEQUENCE_TOKENS + 1, D), jnp.float32)
    moe_total, _ = lax.scan(per_expert, start_total, jnp.arange(EXPERTS, dtype=jnp.int32))
    moe = moe_total[:SEQUENCE_TOKENS]
    final = deep_alpha * x_one.astype(jnp.float32) + moe
    return layer_norm_gain(final, norm2_gain).astype(jnp.bfloat16)
```

```python
import functools

import jax
import jax.numpy as jnp
import numpy as np
from jax import lax
from jax.experimental import pallas as pl
from jax.experimental.pallas import tpu as pltpu
from jax.sharding import PartitionSpec as P

GRID_W = 64


deep_alpha = 2.0**0.5
rope_theta = 10000.0


def rotation_table(tokens, half):
    freq = rope_theta ** (-np.arange(0, half, 2, dtype=np.float64) / half)
    blank = np.zeros((1, half // 2))
    rows = np.arange(tokens // GRID_W, dtype=np.float64)[:, None] * freq
    cols = np.arange(GRID_W, dtype=np.float64)[:, None] * freq

    def spread(angles, first):
        empty = np.broadcast_to(blank, angles.shape)
        place = (lambda v: [v, empty]) if first else (lambda v: [empty, v])
        cosine, sine = np.cos(angles), np.sin(angles)
        return [
            np.concatenate(place(cosine) + place(cosine), 1),
            np.concatenate(place(-sine) + place(sine), 1),
        ]

    return np.concatenate(spread(rows, True) + spread(cols, False), 0).astype(np.float32)


def rotate_block(block, gain, cosine, sine):
    values32 = block.astype(jnp.float32)
    normed = values32 * lax.rsqrt(jnp.mean(values32 * values32, -1, keepdims=True) + 1e-06) * gain
    half = normed.shape[-1] // 2
    return (normed * cosine + pltpu.roll(normed, half, 1) * sine).astype(jnp.bfloat16)


MESH = pl.DeviceIdType.MESH


def flip_bits(a, b, size):
    out = 0
    bit = 1
    while bit < size:
        out = out + ((a // bit + b // bit) % 2) * bit
        bit *= 2
    return out


def at_sp(index):
    return {"sp": index}


def at_tp(index):
    return {"tp": index}


def tp_partners(n_tp):
    t = lax.axis_index("tp")
    t1 = t + 1 - 2 * (t % 2)
    t2 = (t + n_tp // 2) % n_tp
    t3 = (t1 + n_tp // 2) % n_tp
    return t, t1, t2, t3


def attn_kernel(
    n_sp,
    n_tp,
    heads,
    kv_heads,
    width,
    cap,
    experts_total,
    exponent_scale,
    table,
    q_in,
    k_in,
    v_in,
    q_gain,
    k_gain,
    pack,
    gain,
    resid_hbm,
    w_hbm,
    down_hbm,
    x_out,
    outgoing,
    meta,
    down_cols,
    slots,
    q_ref,
    m_s,
    l_s,
    acc,
    attn,
    w,
    resid,
    place,
    part,
    from_core,
    from_pair,
    pair_sum,
    z,
    local,
    send,
    recv,
    sum_send,
    sum_recv,
    down_send,
    down_recv,
):
    me = lax.axis_index("sp")
    t, t1, t2, t3 = tp_partners(n_tp)
    pair = me + 1 - 2 * (me % 2)
    group = heads // kv_heads
    tokens = q_in.shape[0]
    strips, strip = w.shape[0], w.shape[2]
    own = z.shape[1]
    stride = (cap + 7) // 8 * 8

    def load(c):
        return pltpu.make_async_copy(
            w_hbm.at[:, pl.ds(pl.multiple_of(c * strip, strip), strip)], w.at[c], local.at[c]
        )

    def load_resid(c):
        return pltpu.make_async_copy(
            resid_hbm.at[:, pl.ds(pl.multiple_of(c * strip, strip), strip)],
            resid.at[c],
            local.at[strips + c],
        )

    def start_loads(c, _):
        load(c).start()
        load_resid(c).start()
        return 0

    lax.fori_loop(0, strips, start_loads, 0)

    barrier = pltpu.get_barrier_semaphore()
    pl.semaphore_signal(barrier, inc=1, device_id=at_sp(pair), device_id_type=MESH)
    pl.semaphore_signal(barrier, inc=1, device_id=at_tp(t1), device_id_type=MESH)
    pl.semaphore_signal(barrier, inc=1, device_id=at_tp(t2), device_id_type=MESH)
    pl.semaphore_signal(barrier, inc=1, device_id=at_tp(t3), device_id_type=MESH)

    def greet(j, _):
        pl.semaphore_signal(
            barrier, inc=1, device_id=at_sp(flip_bits(me, 2 * j, n_sp)), device_id_type=MESH
        )
        return 0

    lax.fori_loop(1, n_sp // 2, greet, 0)

    grid_rows = tokens // GRID_W
    all_rows = (table.shape[0] - 2 * GRID_W) // 2
    kv_ref = slots.at[0]

    def angles(i):
        row = me * grid_rows + i
        cosine = table[pl.ds(row, 1), :] + table[2 * all_rows : 2 * all_rows + GRID_W, :]
        sine = table[pl.ds(all_rows + row, 1), :] + table[2 * all_rows + GRID_W :, :]
        return cosine, sine

    for i in range(grid_rows):
        block = slice(i * GRID_W, (i + 1) * GRID_W)
        cosine, sine = angles(i)
        for g in range(kv_heads):
            lanes = slice(g * width, (g + 1) * width)
            kv_ref[block, lanes] = rotate_block(k_in[block, lanes], k_gain[...], cosine, sine)
    kv_ref[:, kv_heads * width :] = v_in[...]
    pl.semaphore_wait(barrier, n_sp // 2 + 3)

    def copy(src, slot, target):
        return pltpu.make_async_remote_copy(
            src_ref=src,
            dst_ref=slots.at[slot],
            send_sem=send.at[slot],
            recv_sem=recv.at[slot],
            device_id=at_sp(target),
            device_id_type=MESH,
        )

    copy(kv_ref, 1, pair).start()

    def spread(j, _):
        copy(kv_ref, 2 * j, flip_bits(me, 2 * j, n_sp)).start()
        return 0

    lax.fori_loop(1, n_sp // 2, spread, 0)

    share = down_cols.shape[2]

    def down_copy(j):
        target = (t1, t2, t3)[j]
        return pltpu.make_async_remote_copy(
            src_ref=down_hbm.at[:, pl.ds(pl.multiple_of(target * share, share), share)],
            dst_ref=down_cols.at[t],
            send_sem=down_send.at[j],
            recv_sem=down_recv.at[j],
            device_id=at_tp(target),
            device_id_type=MESH,
        )

    for j in range(3):
        down_copy(j).start()

    for i in range(grid_rows):
        block = slice(i * GRID_W, (i + 1) * GRID_W)
        cosine, sine = angles(i)
        for h in range(heads):
            lanes = slice(h * width, (h + 1) * width)
            q_ref[block, lanes] = rotate_block(q_in[block, lanes], q_gain[...], cosine, sine)

    m_s[...] = jnp.full(m_s.shape, -1e30, jnp.float32)
    l_s[...] = jnp.zeros(l_s.shape, jnp.float32)
    acc[...] = jnp.zeros(acc.shape, jnp.float32)

    def process(block):
        for h in range(heads):
            g = h // group
            q = q_ref[:, h * width : (h + 1) * width]
            k = block[:, g * width : (g + 1) * width]
            v = block[:, (kv_heads + g) * width : (kv_heads + g + 1) * width]
            s = lax.dot_general(q, k, (((1,), (1,)), ((), ())), preferred_element_type=jnp.float32)
            m_prev = m_s[h]
            m_new = jnp.maximum(m_prev, jnp.max(s, -1, keepdims=True))
            m_s[h] = m_new
            alpha = jnp.exp2((m_prev - m_new) * exponent_scale)
            p = jnp.exp2((s - m_new[:, :1]) * exponent_scale)
            l_s[h] = l_s[h] * alpha + jnp.sum(p, -1, keepdims=True)
            acc[h] = acc[h] * alpha + jnp.dot(
                p.astype(jnp.bfloat16), v, preferred_element_type=jnp.float32
            )

    process(kv_ref)

    lane = lax.broadcasted_iota(jnp.int32, (own, 128), 1).astype(jnp.float32)
    e0, e1 = pack[:, 0:1], pack[:, 1:2]
    named0 = jnp.where(lane == e0, 1.0, 0.0)
    named1 = jnp.where(lane == e1, 1.0, 0.0)
    before = (
        lax.broadcasted_iota(jnp.int32, (own, own), 0)
        > lax.broadcasted_iota(jnp.int32, (own, own), 1)
    )
    before = jnp.where(before, 1.0, 0.0).astype(jnp.bfloat16)
    earlier = jnp.dot(
        before, (named0 + named1).astype(jnp.bfloat16), preferred_element_type=jnp.float32
    )
    slot0 = e0 * stride + jnp.sum(earlier * named0, -1, keepdims=True)
    slot1 = e1 * stride + jnp.sum(earlier * named1, -1, keepdims=True)
    column = lax.broadcasted_iota(jnp.int32, place.shape, 1).astype(jnp.float32)
    place[...] = jnp.where(
        column == slot0, 1.0, jnp.where(column == slot1, 1.0, 0.0)
    ).astype(jnp.bfloat16)
    meta[...] = jnp.where(
        lane == 0.0,
        slot0,
        jnp.where(lane == 1.0, slot1, jnp.where(lane == 2.0, pack[:, 2:3], pack[:, 3:4])),
    )

    def step(j, _):
        even = 2 * j + 2
        copy(kv_ref, even, pair).wait_recv()
        copy(slots.at[even], even + 1, pair).start()
        copy(kv_ref, even - 1, pair).wait_recv()
        process(slots.at[even - 1])
        process(slots.at[even])
        return 0

    lax.fori_loop(0, n_sp // 2 - 1, step, 0)
    copy(kv_ref, n_sp - 1, pair).wait_recv()
    process(slots.at[n_sp - 1])
    for h in range(heads):
        attn[:, h * width : (h + 1) * width] = (acc[h] / l_s[h]).astype(jnp.bfloat16)

    def sum_copy(src, dst, kind, c, target):
        return pltpu.make_async_remote_copy(
            src_ref=src,
            dst_ref=dst,
            send_sem=sum_send.at[kind, c],
            recv_sem=sum_recv.at[kind, c],
            device_id=at_tp(target),
            device_id_type=MESH,
        )

    def core_copy(c, half):
        return sum_copy(part.at[c, t3 if half else t1], from_core.at[c, half], half, c, t1)

    def pair_copy(c):
        return sum_copy(pair_sum.at[c], from_pair.at[c], 2, c, t2)

    def project(c):
        load(c).wait()
        y = jnp.dot(attn[...], w[c], preferred_element_type=jnp.float32)
        for i in range(n_tp):
            part[c, i] = y[i * own : (i + 1) * own].astype(jnp.bfloat16)
        core_copy(c, 1).start()
        core_copy(c, 0).start()

    def add_pair(c):
        core_copy(c, 1).wait_recv()
        pair_sum[c] = (
            part[c, t2].astype(jnp.float32) + from_core[c, 1].astype(jnp.float32)
        ).astype(jnp.bfloat16)
        pair_copy(c).start()

    depth = min(4, strips)

    def reduce_step(c, _):
        @pl.when(c < strips)
        def _():
            project(c)

        @pl.when(c >= depth)
        def _():
            add_pair(c - depth)

        return 0

    lax.fori_loop(0, strips + depth, reduce_step, 0)

    def finish(c, total):
        core_copy(c, 0).wait_recv()
        pair_copy(c).wait_recv()
        load_resid(c).wait()
        proj = (
            part[c, t].astype(jnp.float32)
            + from_core[c, 0].astype(jnp.float32)
            + from_pair[c].astype(jnp.float32)
        ).astype(jnp.bfloat16)
        summed = deep_alpha * resid[c].astype(jnp.float32) + proj.astype(jnp.float32)
        z[c] = summed
        return total + jnp.sum(summed, -1, keepdims=True)

    features = strips * strip
    mean = lax.fori_loop(0, strips, finish, jnp.zeros((own, 1), jnp.float32)) / features

    def deviate(c, total):
        centre = z[c] - mean
        return total + jnp.sum(centre * centre, -1, keepdims=True)

    spread_sum = lax.fori_loop(0, strips, deviate, jnp.zeros((own, 1), jnp.float32))
    scale = lax.rsqrt(spread_sum / features + 1e-06)

    for c in range(strips):
        cols = slice(c * strip, (c + 1) * strip)
        x = ((z[c] - mean) * scale * gain[:, cols]).astype(jnp.bfloat16)
        x_out[:, cols] = x
        rows = lax.dot_general(
            place[...], x, (((0,), (0,)), ((), ())), preferred_element_type=jnp.float32
        )
        for e in range(experts_total):
            outgoing[e, :, cols] = rows[e * stride : e * stride + cap].astype(jnp.bfloat16)

    def drain(slot, _):
        copy(kv_ref, slot, pair).wait_send()
        return 0

    lax.fori_loop(1, n_sp, drain, 0)

    def drain_sum(c, _):
        core_copy(c, 0).wait_send()
        core_copy(c, 1).wait_send()
        pair_copy(c).wait_send()
        return 0

    lax.fori_loop(0, strips, drain_sum, 0)
    for j in range(3):
        down_copy(j).wait()


def attend(
    queries,
    keys,
    values,
    q_gain,
    k_gain,
    pack,
    gain,
    resid,
    out_weight,
    down_proj,
    n_sp,
    n_tp,
    experts_total,
    cap,
):
    tokens, q_width = queries.shape
    width = q_gain.shape[-1]
    heads, kv_heads = q_width // width, keys.shape[1] // width
    own, features = resid.shape
    strip = 512 if features % 512 == 0 else features
    strips = features // strip
    stride = (cap + 7) // 8 * 8
    table = rotation_table(tokens * n_sp, width // 2)
    chunk = (strips, own, strip)
    vmem = pl.BlockSpec(memory_space=pltpu.VMEM)
    anywhere = pl.BlockSpec(memory_space=pl.ANY)
    return pl.pallas_call(
        functools.partial(
            attn_kernel,
            n_sp,
            n_tp,
            heads,
            kv_heads,
            width,
            cap,
            experts_total,
            width ** (-0.5) * 1.4426950408889634,
        ),
        out_shape=(
            jax.ShapeDtypeStruct((own, features), jnp.bfloat16),
            jax.ShapeDtypeStruct((experts_total, cap, features), jnp.bfloat16),
            jax.ShapeDtypeStruct((own, 128), jnp.float32),
            jax.ShapeDtypeStruct((n_tp, down_proj.shape[0], features // n_tp), jnp.bfloat16),
        ),
        in_specs=[vmem] * 8 + [anywhere] * 3,
        out_specs=(vmem, vmem, vmem, anywhere),
        scratch_shapes=[
            pltpu.VMEM((n_sp, tokens, 2 * kv_heads * width), jnp.bfloat16),
            pltpu.VMEM((tokens, q_width), jnp.bfloat16),
            pltpu.VMEM((heads, tokens, 128), jnp.float32),
            pltpu.VMEM((heads, tokens, 128), jnp.float32),
            pltpu.VMEM((heads, tokens, width), jnp.float32),
            pltpu.VMEM((tokens, q_width), jnp.bfloat16),
            pltpu.VMEM((strips, out_weight.shape[0], strip), jnp.bfloat16),
            pltpu.VMEM(chunk, jnp.bfloat16),
            pltpu.VMEM((own, experts_total * stride), jnp.bfloat16),
            pltpu.VMEM((strips, n_tp, own, strip), jnp.bfloat16),
            pltpu.VMEM((strips, 2, own, strip), jnp.bfloat16),
            pltpu.VMEM(chunk, jnp.bfloat16),
            pltpu.VMEM(chunk, jnp.bfloat16),
            pltpu.VMEM(chunk, jnp.float32),
            pltpu.SemaphoreType.DMA((2 * strips,)),
            pltpu.SemaphoreType.DMA((n_sp,)),
            pltpu.SemaphoreType.DMA((n_sp,)),
            pltpu.SemaphoreType.DMA((3, strips)),
            pltpu.SemaphoreType.DMA((3, strips)),
            pltpu.SemaphoreType.DMA((3,)),
            pltpu.SemaphoreType.DMA((3,)),
        ],
        compiler_params=pltpu.CompilerParams(collective_id=0, has_side_effects=True),
        name="attend",
    )(jnp.asarray(table), queries, keys, values, q_gain, k_gain, pack, gain, resid, out_weight, down_proj)


def moe_kernel(
    n_sp,
    n_tp,
    stride,
    out_ref,
    meta,
    x_one,
    gain,
    gate_hbm,
    up_hbm,
    down_hbm,
    down_cols,
    final,
    w_gate,
    w_up,
    w_down,
    piece,
    rows,
    hidden,
    answer,
    back,
    metas,
    moe,
    moe_send,
    moe_recv,
    local,
    send,
    recv,
    small_send,
    small_recv,
):
    me = lax.axis_index("sp")
    t, t1, t2, t3 = tp_partners(n_tp)
    peers = (t1, t2, t3)
    cap, width = out_ref.shape[1:]
    strip = 1024 if width % 1024 == 0 else width
    share = w_down.shape[2]
    own = final.shape[0]

    loads = [
        pltpu.make_async_copy(src, dst, local.at[i])
        for i, (src, dst) in enumerate(
            (
                (out_ref.at[me], piece.at[me, t]),
                (gate_hbm, w_gate),
                (up_hbm, w_up),
                (down_hbm.at[:, pl.ds(pl.multiple_of(t * share, share), share)], w_down.at[t]),
                (down_cols.at[t1], w_down.at[t1]),
                (down_cols.at[t2], w_down.at[t2]),
                (down_cols.at[t3], w_down.at[t3]),
            )
        )
    ]
    for load in loads:
        load.start()

    barrier = pltpu.get_barrier_semaphore()
    for peer in peers:
        pl.semaphore_signal(barrier, inc=1, device_id=at_tp(peer), device_id_type=MESH)

    def greet(k, _):
        pl.semaphore_signal(
            barrier, inc=1, device_id=at_sp(flip_bits(me, k, n_sp)), device_id_type=MESH
        )
        return 0

    lax.fori_loop(1, n_sp, greet, 0)
    pl.semaphore_wait(barrier, n_sp + 2)

    def order(i):
        return jnp.where(i < 2, i, 2 + (i - 2 + n_sp // 2 - 2) % max(n_sp - 2, 1))

    def copy(src, dst, kind, k, target):
        return pltpu.make_async_remote_copy(
            src_ref=src,
            dst_ref=dst,
            send_sem=send.at[kind, k],
            recv_sem=recv.at[kind, k],
            device_id=target,
            device_id_type=MESH,
        )

    def owner(k):
        return flip_bits(me, k, n_sp)

    def first_copy(k):
        return copy(out_ref.at[owner(k)], piece.at[me, t], 0, k, at_sp(owner(k)))

    def core_forward(k):
        return copy(piece.at[owner(k), t], piece.at[owner(k), t], 1, k, at_tp(t1))

    def pair_forward(k):
        return copy(piece.at[owner(k), t], piece.at[owner(k), t], 2, k, at_tp(t2))

    def relay_copy(k):
        return copy(piece.at[owner(k), t2], piece.at[owner(k), t2], 3, k, at_tp(t1))

    def hidden_copy(k, j):
        return copy(hidden.at[k, t], hidden.at[k, t], 4 + j, k, at_tp(peers[j]))

    def back_copy(k):
        return copy(answer.at[k], back.at[me], 7, k, at_sp(owner(k)))

    def small_copy(src, dst, kind, j):
        return pltpu.make_async_remote_copy(
            src_ref=src,
            dst_ref=dst,
            send_sem=small_send.at[kind, j],
            recv_sem=small_recv.at[kind, j],
            device_id=at_tp(peers[j]),
            device_id_type=MESH,
        )

    def meta_copy(j):
        return small_copy(meta, metas.at[t], 0, j)

    def moe_copy(j):
        return small_copy(moe_send.at[peers[j]], moe_recv.at[t], 1, j)

    copy(out_ref.at[me], piece.at[me, t], 2, 0, at_tp(t2)).start()
    copy(out_ref.at[me], piece.at[me, t], 1, 0, at_tp(t1)).start()

    def spread(i, _):
        first_copy(order(i)).start()
        return 0

    lax.fori_loop(1, n_sp, spread, 0)
    for j in range(3):
        meta_copy(j).start()
    metas[t] = meta[...]
    rows[...] = jnp.zeros(rows.shape, jnp.float32)
    moe[...] = jnp.zeros(moe.shape, jnp.float32)
    for load in loads:
        load.wait()

    def stage_forward(k):
        first_copy(k).wait_recv()
        pair_forward(k).start()
        core_forward(k).start()

    def stage_relay(k):
        pair_forward(k).wait_recv()
        relay_copy(k).start()

    def stage_expert(k):
        core_forward(k).wait_recv()
        relay_copy(k).wait_recv()
        source = owner(k)
        for lane in range(n_tp):
            rows[lane * stride : lane * stride + cap, :] = piece[source, lane].astype(jnp.float32)
        gate = jnp.zeros((n_tp * stride, w_gate.shape[1]), jnp.float32)
        up = jnp.zeros((n_tp * stride, w_up.shape[1]), jnp.float32)
        for c in range(0, width, strip):
            x = rows[:, c : c + strip].astype(jnp.bfloat16)
            gate += jnp.dot(x, w_gate[c : c + strip, :], preferred_element_type=jnp.float32)
            up += jnp.dot(x, w_up[c : c + strip, :], preferred_element_type=jnp.float32)
        hidden[k, t] = (gate / (1.0 + jnp.exp(-gate)) * up).astype(jnp.bfloat16)
        for j in (1, 2, 0):
            hidden_copy(k, j).start()

    def stage_down(k):
        for j in range(3):
            hidden_copy(k, j).wait_recv()
        y = jnp.zeros((n_tp * stride, share), jnp.float32)
        for s in range(n_tp):
            y += jnp.dot(hidden[k, s], w_down[s], preferred_element_type=jnp.float32)

        def put(dst, row):
            for lane in range(n_tp):
                dst[row, lane] = y[lane * stride : lane * stride + cap].astype(jnp.bfloat16)

        @pl.when(k == 0)
        def _():
            put(back, me)

        @pl.when(k > 0)
        def _():
            put(answer, k)
            back_copy(k).start()

    def tick(i, _):
        @pl.when(jnp.logical_and(i >= 1, i < n_sp))
        def _():
            stage_forward(order(i))

        @pl.when(jnp.logical_and(i >= 1, i < n_sp + 1))
        def _():
            stage_relay(order(i - 1))

        @pl.when(i >= 2)
        def _():
            stage_down(order(i - 2))

        @pl.when(jnp.logical_and(i >= 1, i < n_sp + 1))
        def _():
            stage_expert(order(i - 1))

        return 0

    lax.fori_loop(0, n_sp + 2, tick, 0)

    for j in range(3):
        meta_copy(j).wait_recv()

    column = lax.broadcasted_iota(jnp.int32, (own, n_tp * stride), 1).astype(jnp.float32)

    def gather(k):
        source = owner(k)
        for lane in range(n_tp):
            rows[lane * stride : lane * stride + cap, :share] = back[source, lane].astype(
                jnp.float32
            )
        return rows[:, :share].astype(jnp.bfloat16), source

    def weigh(taken, source, lane):
        about = metas[lane]
        low = (source * stride).astype(jnp.float32)
        shift = ((lane - source) * stride).astype(jnp.float32)
        weight = jnp.zeros(column.shape, jnp.float32)
        for choice in range(2):
            slot = about[:, choice : choice + 1]
            inside = jnp.logical_and(slot >= low, slot < low + stride)
            target = jnp.where(inside, slot + shift, -1.0)
            weight += jnp.where(column == target, about[:, 2 + choice : 3 + choice], 0.0)
        high = weight.astype(jnp.bfloat16)
        low_part = (weight - high.astype(jnp.float32)).astype(jnp.bfloat16)
        both = jnp.concatenate([high, low_part], 0)
        picked = jnp.dot(both, taken, preferred_element_type=jnp.float32)
        return moe[lane] + (picked[:own] + picked[own:])

    def combine(i, _):
        k = order(i)

        @pl.when(k > 0)
        def _():
            back_copy(k).wait_recv()

        taken, source = gather(k)
        for lane in range(n_tp):
            moe[lane] = weigh(taken, source, lane)
        return 0

    lax.fori_loop(0, n_sp - 1, combine, 0)
    last = order(n_sp - 1)
    back_copy(last).wait_recv()
    taken, source = gather(last)
    for j in (1, 2, 0):
        moe_send[peers[j]] = weigh(taken, source, peers[j]).astype(jnp.bfloat16)
        moe_copy(j).start()
    mine = weigh(taken, source, t)

    def add(lane, value):
        cols = pl.ds(pl.multiple_of(lane * share, share), share)
        summed = deep_alpha * x_one[:, cols].astype(jnp.float32) + value
        moe[lane] = summed
        return jnp.sum(summed, -1, keepdims=True)

    total = add(t, mine)
    for j in range(3):
        moe_copy(j).wait_recv()
        total += add(peers[j], moe_recv[peers[j]].astype(jnp.float32))
    mean = total / width
    spread_sum = jnp.zeros((own, 1), jnp.float32)
    for s in range(n_tp):
        centre = moe[s] - mean
        spread_sum += jnp.sum(centre * centre, -1, keepdims=True)
    scale = lax.rsqrt(spread_sum / width + 1e-06)
    for s in range(n_tp):
        cols = slice(s * share, (s + 1) * share)
        final[:, cols] = ((moe[s] - mean) * scale * gain[:, cols]).astype(jnp.bfloat16)

    def drain(k, _):
        core_forward(k).wait_send()
        pair_forward(k).wait_send()
        relay_copy(k).wait_send()
        for j in range(3):
            hidden_copy(k, j).wait_send()
        return 0

    lax.fori_loop(0, n_sp, drain, 0)

    def drain_far(k, _):
        first_copy(k).wait_send()
        back_copy(k).wait_send()
        return 0

    lax.fori_loop(1, n_sp, drain_far, 0)
    for j in range(3):
        meta_copy(j).wait_send()
        moe_copy(j).wait_send()


def experts(outgoing, meta, x_one, gain, gate_proj, up_proj, down_proj, down_cols, n_sp, n_tp):
    cap, features = outgoing.shape[1:]
    stride = (cap + 7) // 8 * 8
    own = x_one.shape[0]
    share = features // n_tp
    hidden_share = gate_proj.shape[1]
    vmem = pl.BlockSpec(memory_space=pltpu.VMEM)
    anywhere = pl.BlockSpec(memory_space=pl.ANY)
    slots = pltpu.VMEM((n_sp, n_tp, cap, share), jnp.bfloat16)
    split = pltpu.VMEM((n_tp, own, share), jnp.bfloat16)
    return pl.pallas_call(
        functools.partial(moe_kernel, n_sp, n_tp, stride),
        out_shape=jax.ShapeDtypeStruct((own, features), jnp.bfloat16),
        in_specs=[vmem] * 4 + [anywhere] * 4,
        out_specs=vmem,
        scratch_shapes=[
            pltpu.VMEM(gate_proj.shape, jnp.bfloat16),
            pltpu.VMEM(up_proj.shape, jnp.bfloat16),
            pltpu.VMEM(down_cols.shape, jnp.bfloat16),
            pltpu.VMEM((n_sp, n_tp, cap, features), jnp.bfloat16),
            pltpu.VMEM((n_tp * stride, features), jnp.float32),
            pltpu.VMEM((n_sp, n_tp, n_tp * stride, hidden_share), jnp.bfloat16),
            slots,
            slots,
            pltpu.VMEM((n_tp,) + meta.shape, jnp.float32),
            pltpu.VMEM((n_tp, own, share), jnp.float32),
            split,
            split,
            pltpu.SemaphoreType.DMA((7,)),
            pltpu.SemaphoreType.DMA((8, n_sp)),
            pltpu.SemaphoreType.DMA((8, n_sp)),
            pltpu.SemaphoreType.DMA((2, 3)),
            pltpu.SemaphoreType.DMA((2, 3)),
        ],
        compiler_params=pltpu.CompilerParams(collective_id=1, has_side_effects=True),
        name="experts",
    )(outgoing, meta, x_one, gain, gate_proj, up_proj, down_proj, down_cols)


def per_device(
    resid,
    queries,
    keys,
    values,
    q_gain,
    key_norm_gain,
    out_weight,
    norm1_gain,
    norm2_gain,
    expert_ids,
    group_weight,
    expert_weight,
    gate_proj,
    up_proj,
    down_proj,
):
    lanes = lax.axis_size("tp")
    sp_count = lax.axis_size("sp")
    own_rows, model_width = resid.shape
    top_count = expert_ids.shape[1]
    expert_local = gate_proj.shape[0]
    expert_total = expert_local * sp_count
    capacity = (3 * top_count * own_rows + 2 * expert_total - 1) // (2 * expert_total)
    gates = group_weight[:, None] * expert_weight / jnp.sum(expert_weight, -1, keepdims=True)
    pack = jnp.concatenate([expert_ids.astype(jnp.float32), gates], 1)
    down_local = down_proj.reshape(down_proj.shape[1:])
    x_one, outgoing, meta, down_cols = attend(
        queries,
        keys,
        values,
        q_gain[None, :],
        key_norm_gain[None, :],
        pack,
        norm1_gain[None, :],
        resid,
        out_weight,
        down_local,
        sp_count,
        lanes,
        expert_total,
        capacity,
    )
    return experts(
        outgoing.reshape(sp_count, expert_local * capacity, model_width),
        meta,
        x_one,
        norm2_gain[None, :],
        gate_proj.reshape(gate_proj.shape[1:]),
        up_proj.reshape(up_proj.shape[1:]),
        down_local,
        down_cols,
        sp_count,
        lanes,
    )


def solution(mesh):
    in_specs = (
        P(("sp", "tp"), None),
        P("sp", "tp"),
        P("sp", "tp"),
        P("sp", "tp"),
        P(),
        P(),
        P("tp", None),
        P(),
        P(),
        P(("sp", "tp"), None),
        P(("sp", "tp")),
        P(("sp", "tp"), None),
        P("sp", None, "tp"),
        P("sp", None, "tp"),
        P("sp", "tp", None),
    )
    out_specs = P(("sp", "tp"), None)
    return jax.shard_map(
        per_device, mesh=mesh, in_specs=in_specs, out_specs=out_specs, check_vma=False
    )
```
